32 devices in a mesh: grp: 2 (over y), fs: 4 (over z), tp: 4 (over x, core).
Axes of the slice: x: 2, y: 2, z: 4, core: 2. Of those that a mesh axis runs over, the one named last changes fastest.
Arguments:
- tokens: bfloat16 [2048, 2048], P(('grp', 'fs')), parts along dimension 0, may hold values from -6 to 6
- decay_logs: float32 [8, 2048], P('tp', ('grp', 'fs')), parts along dimension 1, may hold values from -1.5 to 0, as said below
- query_weight: float32 [2048, 1024], P('fs', 'tp'), may hold values from -0.125 to 0.125
- key_weight: float32 [2048, 1024], P('fs', 'tp'), may hold values from -0.125 to 0.125
- value_weight: float32 [2048, 2048], P('fs', 'tp'), may hold values from -0.125 to 0.125
- out_weight: float32 [2048, 2048], P('tp', 'fs'), may hold values from -0.125 to 0.125
- gate_weight: float32 [2048, 5632], P('fs', 'tp'), may hold values from -0.125 to 0.125
- up_weight: float32 [2048, 5632], P('fs', 'tp'), may hold values from -0.125 to 0.125
- down_weight: float32 [5632, 2048], P('tp', 'fs'), may hold values from -0.078125 to 0.078125
- query_scale: float32 [1024], P(('tp', 'fs')), may hold values from 0.5 to 2
- key_scale: float32 [1024], P(('tp', 'fs')), may hold values from 0.5 to 2
- value_scale: float32 [2048], P(('tp', 'fs')), may hold values from 0.5 to 2
- out_scale: float32 [2048], P('fs'), may hold values from 0.5 to 2
- gate_scale: float32 [5632], P(('tp', 'fs')), may hold values from 0.5 to 2
- up_scale: float32 [5632], P(('tp', 'fs')), may hold values from 0.5 to 2
- down_scale: float32 [2048], P('fs'), may hold values from 0.5 to 2
- conv_weight: float32 [3, 5632], P(None, 'tp'), may hold values from -3.5 to 3.5
- conv_bias: float32 [5632], P('tp'), may hold values from -3 to 3
- first_gain: float32 [2048], replicated, may hold values from 0.1 to 1.9
- first_bias: float32 [2048], replicated, may hold values from -3 to 3
- second_gain: float32 [2048], replicated, may hold values from 0.1 to 1.9
- second_bias: float32 [2048], replicated, may hold values from -3 to 3
Outputs:
- layer_out: bfloat16 [2048, 2048], P(('grp', 'fs', 'tp')), parts along dimension 0
The draws below stay inside these ranges and needn't reach their ends.
There are 2 independent parts, one for each index of `grp`. The reference program is written for one: setup_inputs(seed, part) draws one part's arguments, and reference() takes and returns one part's arrays. A program takes and returns all parts, laid end to end along the dimension named above; an argument that names none is the same for every part. Nothing has to cross between parts.
Inputs may be any that keep to these rules, and one draw needn't show every extreme that they name: `decay_logs`: log-decays are negative; each head's rate is steady along a sequence except at a few positions.
All inputs are finite; a program needn't handle non-finite values.
Results may differ from the reference program's by a relative error of at most 0.018.
Values may be sent and summed in bfloat16 or wider, within the bound.
No kernel may reach another device: no remote copies, remote signals or barrier semaphores. Data moves between devices by JAX's collectives and lax.ppermute only.
A program may use at most 64 MiB of HBM per device.

```python
import math
import jax
import jax.numpy as jnp
from jax import lax

D = 2048
RETENTION_HEADS = 8
QK_HEAD = 128
V_HEAD = 256
FF = 5632
SEQUENCE_TOKENS = 256
BLOCK = 128
KERNEL = 3
QK_WIDTH = 1024
V_WIDTH = 2048
TOTAL_TOKENS = 1024
N_TP = 4


def draw_decay_logs(key, part):
    random_subkeys = jax.random.split(jax.random.fold_in(key, 17), 6)
    sequence_list = TOTAL_TOKENS // SEQUENCE_TOKENS
    quick_share = 0.5
    quick_heads = jax.random.uniform(random_subkeys[0], (RETENTION_HEADS, 1, 1)) < quick_share
    quick_rate = 1.0 / jax.random.uniform(random_subkeys[1], (RETENTION_HEADS, 1, 1), minval=30.0, maxval=100.0)
    slow_rate = math.log(10.0) * jax.random.uniform(random_subkeys[2], (RETENTION_HEADS, 1, 1), minval=0.1, maxval=0.3) / SEQUENCE_TOKENS
    factor = jnp.exp(jax.random.uniform(random_subkeys[3], (1, sequence_list, 1), minval=0.0, maxval=math.log(2.5)))
    baseline_level = -jnp.where(quick_heads, quick_rate, slow_rate) * factor
    spike_positions = jax.random.randint(random_subkeys[4], (RETENTION_HEADS, sequence_list, 2, 1), 0, SEQUENCE_TOKENS)
    spike_logarithms = jnp.log(jax.random.uniform(random_subkeys[5], (RETENTION_HEADS, sequence_list, 2, 1), minval=0.5, maxval=0.8))
    spike_present = jnp.arange(SEQUENCE_TOKENS)[None, None, None, :] == spike_positions
    spike_events = jnp.sum(jnp.where(spike_present, spike_logarithms, 0.0), axis=2)
    return (baseline_level + spike_events).reshape(RETENTION_HEADS, TOTAL_TOKENS).astype(jnp.float32)


def block_levels(own_key, shape, shards, smallest, largest):
    level, own = 1.0, jax.random.fold_in(own_key, 6)
    for axis_at, shards_of in shards:
        draws = jnp.exp(jax.random.uniform(jax.random.fold_in(own, axis_at), (shards_of,), jnp.float32, smallest / len(shards), largest / len(shards)))
        level = level * jnp.repeat(draws, shape[axis_at] // shards_of).reshape([-1 if axis == axis_at else 1 for axis in range(len(shape))])
    return level


def normal_values(rng, shape, deviation, most, shards=(), held_as=jnp.bfloat16):
    array = jax.random.normal(rng, shape, jnp.float32) * deviation
    if len(shards) > 0:
        array = block_levels(rng, shape, shards, -0.22, 0.18) * array
    return jnp.clip(array, min=-most, max=most).astype(held_as)


def setup_inputs(seed: int = 0, part: int = 0) -> dict:
    key_of = jax.random.split(jax.random.key(seed), 23)
    part_splits = jax.random.split(jax.random.fold_in(key_of[22], part), 23)
    return {
        "tokens": normal_values(part_splits[0], (TOTAL_TOKENS, D), 1.0, 6.0, ((0, 4),)),
        "decay_logs": draw_decay_logs(jax.random.fold_in(jax.random.fold_in(key_of[22], part), 71), part),
        "query_weight": normal_values(key_of[2], (D, QK_WIDTH), D ** -0.5, 0.125, ((0, 4), (1, 4)), jnp.float32),
        "key_weight": normal_values(key_of[3], (D, QK_WIDTH), D ** -0.5, 0.125, ((0, 4), (1, 4)), jnp.float32),
        "value_weight": normal_values(key_of[4], (D, V_WIDTH), D ** -0.5, 0.125, ((0, 4), (1, 4)), jnp.float32),
        "out_weight": normal_values(key_of[5], (V_WIDTH, D), V_WIDTH ** -0.5, 0.125, ((0, 4), (1, 4)), jnp.float32),
        "gate_weight": normal_values(key_of[6], (D, FF), D ** -0.5, 0.125, ((0, 4), (1, 4)), jnp.float32),
        "up_weight": normal_values(key_of[7], (D, FF), D ** -0.5, 0.125, ((0, 4), (1, 4)), jnp.float32),
        "down_weight": normal_values(key_of[8], (FF, D), FF ** -0.5, 0.078125, ((0, 4), (1, 4)), jnp.float32),
        "query_scale": jnp.clip(jnp.exp(math.log(2.0) - 1.3862944 * jax.random.uniform(key_of[9], (QK_WIDTH,), jnp.float32) ** block_levels(key_of[9], (QK_WIDTH,), ((0, 16),), -0.2, 0.2)), 0.5, 2.0),
        "key_scale": jnp.clip(jnp.exp(math.log(2.0) - 1.3862944 * jax.random.uniform(key_of[10], (QK_WIDTH,), jnp.float32) ** block_levels(key_of[10], (QK_WIDTH,), ((0, 16),), -0.2, 0.2)), 0.5, 2.0),
        "value_scale": jnp.clip(jnp.exp(math.log(2.0) - 1.3862944 * jax.random.uniform(key_of[11], (V_WIDTH,), jnp.float32) ** block_levels(key_of[11], (V_WIDTH,), ((0, 16),), -0.2, 0.2)), 0.5, 2.0),
        "out_scale": jnp.clip(jnp.exp(math.log(2.0) - 1.3862944 * jax.random.uniform(key_of[12], (D,), jnp.float32) ** block_levels(key_of[12], (D,), ((0, 4),), -0.2, 0.2)), 0.5, 2.0),
        "gate_scale": jnp.clip(jnp.exp(math.log(2.0) - 1.3862944 * jax.random.uniform(key_of[13], (FF,), jnp.float32) ** block_levels(key_of[13], (FF,), ((0, 16),), -0.2, 0.2)), 0.5, 2.0),
        "up_scale": jnp.clip(jnp.exp(math.log(2.0) - 1.3862944 * jax.random.uniform(key_of[14], (FF,), jnp.float32) ** block_levels(key_of[14], (FF,), ((0, 16),), -0.2, 0.2)), 0.5, 2.0),
        "down_scale": jnp.clip(jnp.exp(math.log(2.0) - 1.3862944 * jax.random.uniform(key_of[15], (D,), jnp.float32) ** block_levels(key_of[15], (D,), ((0, 4),), -0.2, 0.2)), 0.5, 2.0),
        "conv_weight": normal_values(key_of[16], (KERNEL, FF), KERNEL ** -0.5, 3.5, ((1, 4),), jnp.float32),
        "conv_bias": normal_values(key_of[17], (FF,), 0.5, 3.0, ((0, 4),), jnp.float32),
        "first_gain": jnp.clip(1.0 + 0.18 * jax.random.normal(key_of[18], (D,), jnp.float32), 0.1, 1.9),
        "first_bias": normal_values(key_of[19], (D,), 0.5, 3.0, (), jnp.float32),
        "second_gain": jnp.clip(1.0 + 0.18 * jax.random.normal(key_of[20], (D,), jnp.float32), 0.1, 1.9),
        "second_bias": normal_values(key_of[21], (D,), 0.5, 3.0, (), jnp.float32),
    }


norm_eps = 1e-05
residual_gain = 2.0 ** 0.25
angle_base = 10000.0

def rotate_pairs(inputs):
    length, head_count, head_width = inputs.shape
    spike_positions = jnp.arange(length, dtype=jnp.float32)
    frequency = 1.0 / angle_base ** jnp.linspace(0.0, 1.0, head_width // 2, dtype=jnp.float32)
    angles = spike_positions[:, None] * frequency[None, :]
    cosine = jnp.cos(angles)[:, None, :]
    sine_part = jnp.sin(angles)[:, None, :]
    paired = inputs.reshape(length, head_count, head_width // 2, 2)
    even_part = paired[..., 0]
    odd_part = paired[..., 1]
    turned = jnp.stack([even_part * cosine - odd_part * sine_part, odd_part * cosine + even_part * sine_part], -1)
    return turned.reshape(inputs.shape)

def retain(queries, key_rows, values, decay_logs):
    length, head_count, key_width = queries.shape
    value_width = values.shape[2]
    blocks = length // BLOCK
    highest = lax.Precision.HIGHEST
    query_blocks = queries.reshape(blocks, BLOCK, head_count, key_width).astype(jnp.float32)
    key_blocks = key_rows.reshape(blocks, BLOCK, head_count, key_width).astype(jnp.float32)
    value_blocks = values.reshape(blocks, BLOCK, head_count, value_width).astype(jnp.float32)
    cumulative = jnp.cumsum(decay_logs.reshape(head_count, blocks, BLOCK), axis=2)
    offsets = jnp.arange(BLOCK)
    causal = offsets[:, None] >= offsets[None, :]
    distance = cumulative[:, :, :, None] - cumulative[:, :, None, :]
    damping = jnp.where(causal, jnp.exp(jnp.where(causal, distance, 0.0)), 0.0)
    scores = jnp.einsum('nqhd,nkhd->hnqk', query_blocks, key_blocks, precision=highest)
    weighted = lax.optimization_barrier((scores * damping).astype(jnp.bfloat16)).astype(jnp.float32)
    within = jnp.einsum('hnqk,nkhv->nqhv', weighted, value_blocks, precision=highest)
    to_end = jnp.exp(cumulative[:, :, -1:] - cumulative)
    from_start = jnp.exp(cumulative)
    carried = jnp.zeros((head_count, key_width, value_width), jnp.float32)
    carried_parts = []
    for segment in range(blocks):
        query_decayed = query_blocks[segment] * from_start[:, segment, :].T[:, :, None]
        carried_parts.append(jnp.einsum('qhd,hdv->qhv', query_decayed, carried, precision=highest))
        key_decayed = key_blocks[segment] * to_end[:, segment, :].T[:, :, None]
        update = jnp.einsum('khd,khv->hdv', key_decayed, value_blocks[segment], precision=highest)
        carried = from_start[:, segment, -1][:, None, None] * carried + update
    return (within + jnp.stack(carried_parts)).reshape(length, head_count, value_width)

def head_norm(outputs):
    centred = outputs - lax.optimization_barrier(jnp.mean(outputs, -1, keepdims=True))
    variance = lax.optimization_barrier(jnp.mean(centred * centred, -1, keepdims=True))
    return centred * lax.rsqrt(variance + norm_eps)

def layer_norm(inputs, gain_vector, offset):
    centred = inputs - lax.optimization_barrier(jnp.mean(inputs, -1, keepdims=True))
    variance = lax.optimization_barrier(jnp.mean(centred * centred, -1, keepdims=True))
    return centred * lax.rsqrt(variance + norm_eps) * gain_vector + offset

def partial_rounded(inputs, weight):
    groups = inputs.reshape(inputs.shape[0], N_TP, -1).astype(jnp.float32)
    stacked = weight.reshape(N_TP, -1, weight.shape[1]).astype(jnp.float32)
    partial_value = jnp.einsum('sgc,gcd->gsd', groups, stacked, precision=lax.Precision.HIGHEST)
    rounded = lax.optimization_barrier(partial_value.astype(jnp.bfloat16)).astype(jnp.float32)
    return lax.optimization_barrier(jnp.sum(rounded, axis=0))

def one_sequence(tokens, decay_logs, query_half, key_half, value_half, out_half, gate_half, up_half, down_half, query_scale, key_scale, value_scale, out_scale, gate_scale, up_scale, down_scale, conv_weight, conv_bias, first_gain, first_bias, second_gain, second_bias):
    length = tokens.shape[0]
    query_raw = jnp.dot(tokens, query_half, preferred_element_type=jnp.float32)
    key_raw = jnp.dot(tokens, key_half, preferred_element_type=jnp.float32)
    value_raw = jnp.dot(tokens, value_half, preferred_element_type=jnp.float32)
    queries = rotate_pairs((query_raw * query_scale).reshape(length, RETENTION_HEADS, QK_HEAD)).astype(jnp.bfloat16)
    key_rows = (rotate_pairs((key_raw * key_scale).reshape(length, RETENTION_HEADS, QK_HEAD)) * QK_HEAD ** (-0.5)).astype(jnp.bfloat16)
    values = (value_raw * value_scale).astype(jnp.bfloat16).reshape(length, RETENTION_HEADS, V_HEAD)
    retained = retain(queries, key_rows, values, decay_logs)
    normed = head_norm(retained).astype(jnp.bfloat16).reshape(length, RETENTION_HEADS * V_HEAD)
    branch = partial_rounded(normed, out_half) * out_scale
    first = layer_norm(residual_gain * tokens.astype(jnp.float32) + branch, first_gain, first_bias).astype(jnp.bfloat16)
    gate = jnp.dot(first, gate_half, preferred_element_type=jnp.float32) * gate_scale
    up_part = jnp.dot(first, up_half, preferred_element_type=jnp.float32) * up_scale
    padded = jnp.pad(gate, ((KERNEL - 1, 0), (0, 0)))
    convolved = conv_bias + jnp.zeros_like(gate)
    for tap_index in range(KERNEL):
        convolved = convolved + padded[tap_index:tap_index + length] * conv_weight[tap_index]
    activated = (jax.nn.gelu(convolved, approximate=False) * up_part).astype(jnp.bfloat16)
    feed = partial_rounded(activated, down_half) * down_scale
    return layer_norm(residual_gain * first.astype(jnp.float32) + feed, second_gain, second_bias).astype(jnp.bfloat16)

def reference(tokens, decay_logs, query_weight, key_weight, value_weight, out_weight, gate_weight, up_weight, down_weight, query_scale, key_scale, value_scale, out_scale, gate_scale, up_scale, down_scale, conv_weight, conv_bias, first_gain, first_bias, second_gain, second_bias):
    sequence_list = tokens.shape[0] // SEQUENCE_TOKENS
    token_seqs = tokens.reshape(sequence_list, SEQUENCE_TOKENS, D)
    decay_seqs = decay_logs.reshape(RETENTION_HEADS, sequence_list, SEQUENCE_TOKENS).transpose(1, 0, 2)
    query_half = query_weight.astype(jnp.bfloat16)
    key_half = key_weight.astype(jnp.bfloat16)
    value_half = value_weight.astype(jnp.bfloat16)
    out_half = out_weight.astype(jnp.bfloat16)
    gate_half = gate_weight.astype(jnp.bfloat16)
    up_half = up_weight.astype(jnp.bfloat16)
    down_half = down_weight.astype(jnp.bfloat16)

    def run_one(paired):
        return one_sequence(paired[0], paired[1], query_half, key_half, value_half, out_half, gate_half, up_half, down_half, query_scale, key_scale, value_scale, out_scale, gate_scale, up_scale, down_scale, conv_weight, conv_bias, first_gain, first_bias, second_gain, second_bias)
    outputs = lax.map(run_one, (token_seqs, decay_seqs))
    return outputs.reshape(sequence_list * SEQUENCE_TOKENS, D)
```

```python
import functools

import jax
import jax.numpy as jnp
from jax import lax
from jax.experimental import pallas as pl
from jax.experimental.pallas import tpu as pltpu
from jax.sharding import PartitionSpec as P


QK_HEAD = 128
V_HEAD = 256
BLOCK = 128
KERNEL = 3


norm_eps = 1e-05
residual_gain = 2.0**0.25
angle_base = 10000.0


def rotate_pairs(inputs):
    length, head_count, head_width = inputs.shape
    spike_positions = jnp.arange(length, dtype=jnp.float32)
    frequency = 1.0 / angle_base ** jnp.linspace(0.0, 1.0, head_width // 2, dtype=jnp.float32)
    angles = spike_positions[:, None] * frequency[None, :]
    cosine = jnp.cos(angles)[:, None, :]
    sine_part = jnp.sin(angles)[:, None, :]
    paired = inputs.reshape(length, head_count, head_width // 2, 2)
    even_part = paired[..., 0]
    odd_part = paired[..., 1]
    turned = jnp.stack(
        [even_part * cosine - odd_part * sine_part, odd_part * cosine + even_part * sine_part], -1
    )
    return turned.reshape(inputs.shape)


def retain(queries, key_rows, values, decay_logs):
    length, head_count, key_width = queries.shape
    value_width = values.shape[2]
    blocks = length // BLOCK
    highest = lax.Precision.HIGHEST
    query_blocks = queries.reshape(blocks, BLOCK, head_count, key_width).astype(jnp.float32)
    key_blocks = key_rows.reshape(blocks, BLOCK, head_count, key_width).astype(jnp.float32)
    value_blocks = values.reshape(blocks, BLOCK, head_count, value_width).astype(jnp.float32)
    cumulative = jnp.cumsum(decay_logs.reshape(head_count, blocks, BLOCK), axis=2)
    offsets = jnp.arange(BLOCK)
    causal = offsets[:, None] >= offsets[None, :]
    distance = cumulative[:, :, :, None] - cumulative[:, :, None, :]
    damping = jnp.where(causal, jnp.exp(jnp.where(causal, distance, 0.0)), 0.0)
    scores = jnp.einsum("nqhd,nkhd->hnqk", query_blocks, key_blocks, precision=highest)
    weighted = lax.optimization_barrier((scores * damping).astype(jnp.bfloat16)).astype(jnp.float32)
    within = jnp.einsum("hnqk,nkhv->nqhv", weighted, value_blocks, precision=highest)
    to_end = jnp.exp(cumulative[:, :, -1:] - cumulative)
    from_start = jnp.exp(cumulative)
    carried = jnp.zeros((head_count, key_width, value_width), jnp.float32)
    carried_parts = []
    for segment in range(blocks):
        query_decayed = query_blocks[segment] * from_start[:, segment, :].T[:, :, None]
        carried_parts.append(jnp.einsum("qhd,hdv->qhv", query_decayed, carried, precision=highest))
        key_decayed = key_blocks[segment] * to_end[:, segment, :].T[:, :, None]
        update = jnp.einsum("khd,khv->hdv", key_decayed, value_blocks[segment], precision=highest)
        carried = from_start[:, segment, -1][:, None, None] * carried + update
    return (within + jnp.stack(carried_parts)).reshape(length, head_count, value_width)


def head_norm(outputs):
    centred = outputs - jnp.mean(outputs, -1, keepdims=True)
    variance = jnp.mean(centred * centred, -1, keepdims=True)
    return centred * lax.rsqrt(variance + norm_eps)


def layer_norm(inputs, gain_vector, offset):
    centred = inputs - jnp.mean(inputs, -1, keepdims=True)
    variance = jnp.mean(centred * centred, -1, keepdims=True)
    return centred * lax.rsqrt(variance + norm_eps) * gain_vector + offset


def local(
    tokens,
    decay_logs,
    query_weight,
    key_weight,
    value_weight,
    out_weight,
    gate_weight,
    up_weight,
    down_weight,
    query_scale,
    key_scale,
    value_scale,
    out_scale,
    gate_scale,
    up_scale,
    down_scale,
    conv_weight,
    conv_bias,
    first_gain,
    first_bias,
    second_gain,
    second_bias,
):
    length = tokens.shape[0]
    share = length // lax.axis_size("tp")
    query_factor, key_factor, value_factor, gate_factor, up_factor, out_factor, down_factor = (
        lax.all_gather(query_scale, "fs", axis=0, tiled=True),
        lax.all_gather(key_scale, "fs", axis=0, tiled=True),
        lax.all_gather(value_scale, "fs", axis=0, tiled=True),
        lax.all_gather(gate_scale, "fs", axis=0, tiled=True),
        lax.all_gather(up_scale, "fs", axis=0, tiled=True),
        lax.all_gather(out_scale, "fs", axis=0, tiled=True),
        lax.all_gather(down_scale, "fs", axis=0, tiled=True),
    )
    query_half = query_weight.astype(jnp.bfloat16)
    key_half = key_weight.astype(jnp.bfloat16)
    value_half = value_weight.astype(jnp.bfloat16)
    out_half = out_weight.astype(jnp.bfloat16)
    gate_half = gate_weight.astype(jnp.bfloat16)
    up_half = up_weight.astype(jnp.bfloat16)
    down_half = down_weight.astype(jnp.bfloat16)
    query_full, key_full, value_full = (
        lax.all_gather(query_half, "fs", axis=0, tiled=True),
        lax.all_gather(key_half, "fs", axis=0, tiled=True),
        lax.all_gather(value_half, "fs", axis=0, tiled=True),
    )
    query_raw = jnp.dot(tokens, query_full, preferred_element_type=jnp.float32)
    key_raw = jnp.dot(tokens, key_full, preferred_element_type=jnp.float32)
    value_raw = jnp.dot(tokens, value_full, preferred_element_type=jnp.float32)
    head_count = query_raw.shape[1] // QK_HEAD
    queries = rotate_pairs((query_raw * query_factor).reshape(length, head_count, QK_HEAD)).astype(
        jnp.bfloat16
    )
    key_rows = (
        rotate_pairs((key_raw * key_factor).reshape(length, head_count, QK_HEAD))
        * QK_HEAD ** (-0.5)
    ).astype(jnp.bfloat16)
    values = (value_raw * value_factor).astype(jnp.bfloat16).reshape(length, head_count, V_HEAD)
    retained = retain(queries, key_rows, values, decay_logs)
    normed = head_norm(retained).astype(jnp.bfloat16).reshape(length, head_count * V_HEAD)
    out_full = lax.all_gather(out_half, "fs", axis=1, tiled=True)
    picked = normed
    branch = (
        lax.psum_scatter(
            jnp.dot(picked, out_full, preferred_element_type=jnp.float32).astype(jnp.bfloat16),
            "tp",
            scatter_dimension=0,
            tiled=True,
        ).astype(jnp.float32)
        * out_factor
    )
    own_rows = lax.dynamic_slice_in_dim(tokens, lax.axis_index("tp") * share, share, 0)
    first = layer_norm(
        residual_gain * own_rows.astype(jnp.float32) + branch, first_gain, first_bias
    ).astype(jnp.bfloat16)
    first_all = lax.all_gather(first, "tp", axis=0, tiled=True)
    gate_full, up_full = (
        lax.all_gather(gate_half, "fs", axis=0, tiled=True),
        lax.all_gather(up_half, "fs", axis=0, tiled=True),
    )
    gate_raw = jnp.dot(first_all, gate_full, preferred_element_type=jnp.float32)
    up_raw = jnp.dot(first_all, up_full, preferred_element_type=jnp.float32)
    gate = gate_raw * gate_factor
    up_part = up_raw * up_factor
    padded = jnp.pad(gate, ((KERNEL - 1, 0), (0, 0)))
    convolved = conv_bias + jnp.zeros_like(gate)
    for tap_index in range(KERNEL):
        convolved = convolved + padded[tap_index : tap_index + length] * conv_weight[tap_index]
    activated = (jax.nn.gelu(convolved, approximate=False) * up_part).astype(jnp.bfloat16)
    down_full = lax.all_gather(down_half, "fs", axis=1, tiled=True)
    picked = activated
    feed = (
        lax.psum_scatter(
            jnp.dot(picked, down_full, preferred_element_type=jnp.float32).astype(jnp.bfloat16),
            "tp",
            scatter_dimension=0,
            tiled=True,
        ).astype(jnp.float32)
        * down_factor
    )
    return layer_norm(
        residual_gain * first.astype(jnp.float32) + feed, second_gain, second_bias
    ).astype(jnp.bfloat16)


PLACES = 4
LANES = 128


def ring(step):
    return [(i, (i + step) % PLACES) for i in range(PLACES)]


def exchange(axis_size, flip):
    return [(i, i ^ flip) for i in range(axis_size)]


def swap(value, places=range(PLACES)):
    pairs = [
        (grp * PLACES + place, (1 - grp) * PLACES + place) for grp in range(2) for place in places
    ]
    return lax.ppermute(value, ("grp", "fs"), pairs)


def line_gather(mine, line):
    before = lax.ppermute(mine, "fs", [(0, 1), (1, 2), (2, 3)])
    behind = lax.ppermute(mine, "fs", [(1, 0), (2, 1), (3, 2)])
    right = lax.ppermute(before, "fs", [(1, 2), (2, 3)])
    left = lax.ppermute(behind, "fs", [(1, 0), (2, 1)])
    two = jnp.where(line >= 2, right, left)
    handed = lax.ppermute(two, "fs", [(1, 0), (2, 3)])
    return (
        (two, swap(two)),
        (before, swap(before, (1, 2, 3))),
        (behind, swap(behind, (0, 1, 2))),
        (handed, swap(handed, (0, 3))),
    )


def line_slots(line):
    behind, before = lax.rem(line + 1, PLACES), lax.rem(line + PLACES - 1, PLACES)
    return (
        (lax.rem(line + 2, PLACES), None),
        (before, line > 0),
        (behind, line < PLACES - 1),
        (jnp.where(line == 0, before, behind), (line == 0) | (line == PLACES - 1)),
    )


def when(condition, body):
    if condition is None:
        body()
    else:
        pl.when(condition)(body)


VMEM = pl.BlockSpec(memory_space=pltpu.VMEM)
SMEM = pl.BlockSpec(memory_space=pltpu.SMEM)


def kernel_call(kernel, outputs, where, operands, flops=0, scratch=(), room=16):
    single = not isinstance(outputs, (tuple, list))
    shapes = (outputs,) if single else tuple(outputs)
    size = sum(operand.size * operand.dtype.itemsize for operand in operands)
    call = pl.pallas_call(
        kernel,
        out_shape=shapes,
        in_specs=[SMEM] + [VMEM] * len(operands),
        out_specs=(VMEM,) * len(shapes),
        scratch_shapes=list(scratch),
        compiler_params=pltpu.CompilerParams(vmem_limit_bytes=room * 2**20),
        cost_estimate=pl.CostEstimate(flops=flops or size, bytes_accessed=size, transcendentals=0),
    )
    result = call(where, *operands)
    return result[0] if single else result


def bf16(*shape):
    return jax.ShapeDtypeStruct(shape, jnp.bfloat16)


def f32_dot(left, right):
    return jnp.dot(left, right, preferred_element_type=jnp.float32)


def in_kernel(where, *refs):
    weights, result = refs[:-1], refs[-1]
    start = 0
    for weight in weights:
        wide = weight.shape[1]
        result[:, start : start + wide] = weight[...].astype(jnp.bfloat16)
        start += wide


def half_call(where, other, weights, steps=2):
    rows = weights[0].shape[0] // 2
    wide = sum(weight.shape[1] for weight in weights)
    block = rows // steps

    def from_half(step, where):
        return (lax.rem(where[2] + other, 2) * steps + step, 0)

    return pl.pallas_call(
        in_kernel,
        out_shape=bf16(rows, wide),
        grid_spec=pltpu.PrefetchScalarGridSpec(
            num_scalar_prefetch=1,
            grid=(steps,),
            in_specs=[pl.BlockSpec((block, weight.shape[1]), from_half) for weight in weights],
            out_specs=pl.BlockSpec((block, wide), lambda step, where: (step, 0)),
        ),
        compiler_params=pltpu.CompilerParams(vmem_limit_bytes=60 * 2**20),
        cost_estimate=pl.CostEstimate(
            flops=6 * rows * wide, bytes_accessed=6 * rows * wide, transcendentals=0
        ),
    )(where, *weights)


def gate_kernel(where, gate, up, down, own, other, *rest):
    sends, held = rest[:-1], rest[-1]
    places, rows, wide = held.shape
    hidden = gate.shape[1] // places
    half, narrow = rows // 2, down.shape[1] // 2
    for place in range(places):
        for start, weight in ((0, gate), (wide // 2, up)):
            block = weight[:, place * hidden : (place + 1) * hidden].astype(jnp.bfloat16)
            if hidden < wide // 2:
                fill = jnp.zeros((block.shape[0], wide // 2 - hidden), jnp.bfloat16)
                block = jnp.concatenate([block, fill], 1)
            held[place, :, start : start + wide // 2] = block

    def cut(result, step, grp):
        place = lax.rem(where[0] + step, places)
        result[:half, :] = held[place, pl.ds(pl.multiple_of(grp * half, half), half), :]
        columns = pl.ds(pl.multiple_of(grp * narrow, narrow), narrow)
        for group in range(wide // narrow):
            count = min(LANES, hidden - group * LANES)
            at = slice(group * narrow, (group + 1) * narrow)
            start = pl.multiple_of(place * hidden + group * LANES, 8)
            result[half : half + count, at] = down[pl.ds(start, count), columns].astype(jnp.bfloat16)
            if count < LANES:
                result[half + count : half + LANES, at] = jnp.zeros(
                    (LANES - count, narrow), jnp.bfloat16
                )

    cut(own, 0, where[2])
    cut(other, 0, 1 - where[2])
    for step, send in enumerate(sends):
        cut(send, step + 1, where[2])


def retention_kernel(
    where,
    tokens,
    scales,
    cosine,
    sine,
    cumulative_row,
    cumulative_column,
    mine,
    other,
    *rest,
):
    pieces, (crossing, kept, weights, out_weights, normed) = rest[:-5], rest[-5:]
    half, inner = mine.shape[0], weights.shape[1]
    outer = mine.shape[1] - inner
    line, me, grp = where[0], where[1], where[2]

    def place_pair(chunk, one, two):
        def body():
            for piece, at in ((one, grp), (two, 1 - grp)):
                start = pl.multiple_of((2 * chunk + at) * half, half)
                weights[pl.ds(start, half), :] = piece[:, :inner]
                columns = pl.ds(pl.multiple_of(chunk * outer, outer), outer)
                rows = pl.ds(pl.multiple_of(at * half, half), half)
                out_weights[rows, columns] = piece[:, inner:]

        return body

    place_pair(line, mine, other)()
    for slot, (chunk, counts) in enumerate(line_slots(line)):
        when(counts, place_pair(chunk, pieces[2 * slot], pieces[2 * slot + 1]))

    length = tokens.shape[0]
    heads = cumulative_row.shape[0]
    qk = heads * QK_HEAD
    lanes = lax.broadcasted_iota(jnp.int32, (length, qk), 1)
    even = lax.rem(lanes, 2) == 0

    def turned(at):
        raw = f32_dot(tokens[...], weights[:, at : at + qk]) * scales[:, at : at + qk]
        swapped = jnp.where(even, pltpu.roll(raw, qk - 1, 1), pltpu.roll(raw, 1, 1))
        return raw * cosine[...] + swapped * sine[...]

    queries = turned(0).astype(jnp.bfloat16)
    key_rows = (turned(qk) * QK_HEAD ** (-0.5)).astype(jnp.bfloat16)
    rows = lax.broadcasted_iota(jnp.int32, (length, length), 0)
    columns = lax.broadcasted_iota(jnp.int32, (length, length), 1)
    causal = rows >= columns
    tensors = 4
    share = length // tensors
    for head in range(heads):
        at = 2 * qk + head * V_HEAD
        values = (
            f32_dot(tokens[...], weights[:, at : at + V_HEAD]) * scales[:, at : at + V_HEAD]
        ).astype(jnp.bfloat16)
        own = slice(head * QK_HEAD, (head + 1) * QK_HEAD)
        scores = lax.dot_general(
            queries[:, own],
            key_rows[:, own],
            (((1,), (1,)), ((), ())),
            preferred_element_type=jnp.float32,
        )
        distance = cumulative_column[:, head : head + 1] - cumulative_row[head : head + 1, :]
        damping = jnp.where(causal, jnp.exp(jnp.where(causal, distance, 0.0)), 0.0)
        retained = f32_dot((scores * damping).astype(jnp.bfloat16), values)
        result = head_norm(retained).astype(jnp.bfloat16)
        for block in range(tensors):
            flip = lax.bitwise_xor(me, block)
            odd = lax.rem(flip, 2)
            to = pl.multiple_of((2 * (1 - odd) + flip // 2) * share, share)
            normed[pl.ds(to, share), head * V_HEAD : (head + 1) * V_HEAD] = result[
                block * share : (block + 1) * share
            ]

    for at in range(0, out_weights.shape[1], outer):
        out = f32_dot(normed[...], out_weights[:, at : at + outer])
        crossing[:, at : at + outer] = out[: length // 2].astype(jnp.bfloat16)
        kept[:, at : at + outer] = out[length // 2 :].astype(jnp.bfloat16)


def summed(kept, arrived, rows):
    return kept[rows].astype(jnp.float32) + arrived[rows].astype(jnp.float32)


def norm_kernel(count, where, residual, *refs):
    parts, (factor, gain, offset, result) = refs[:count], refs[count:]
    share = result.shape[0]
    total = parts[0][:share, :].astype(jnp.float32)
    for part in parts[1:]:
        total += part[:share, :].astype(jnp.float32)
    if residual.shape[0] == share:
        held = residual[...]
    else:
        held = residual[pl.ds(pl.multiple_of(where[1] * share, share), share), :]
    inputs = residual_gain * held.astype(jnp.float32) + total * factor[...]
    result[...] = layer_norm(inputs, gain[...], offset[...]).astype(jnp.bfloat16)


def norm_call(where, residual, parts, factor, gain, offset):
    wide = residual.shape[1]
    return kernel_call(
        functools.partial(norm_kernel, len(parts)),
        bf16(*parts[-1].shape),
        where,
        (residual, *parts, factor.reshape(1, wide), gain.reshape(1, wide), offset.reshape(1, wide)),
        flops=64 * residual.size,
    )


def join_kernel(where, mine, other, *rest):
    pieces, (gate_up, down) = rest[:-2], rest[-2:]
    half = mine.shape[0] - LANES
    groups = down.shape[0] // LANES
    narrow = mine.shape[1] // groups
    for step in range(PLACES):
        pair = (mine, other) if step == 0 else pieces[2 * step - 2 : 2 * step]
        chunk = lax.rem(where[0] - step + PLACES, PLACES)
        for piece, at in zip(pair, (where[2], 1 - where[2])):
            rows = pl.ds(pl.multiple_of((2 * chunk + at) * half, half), half)
            gate_up[rows, :] = piece[:half, :]
            columns = pl.ds(pl.multiple_of((2 * chunk + at) * narrow, narrow), narrow)
            for group in range(groups):
                down[group * LANES : (group + 1) * LANES, columns] = piece[
                    half:, group * narrow : (group + 1) * narrow
                ]


def feed_kernel(
    where,
    own_rows,
    far_rows,
    core_rows,
    far_core_rows,
    gate_up,
    down,
    units,
    crossing,
    kept,
    rows_held,
    active_held,
):
    share = own_rows.shape[0]
    me = where[1]
    hidden = units.shape[1]
    gate_scale, up_scale = units[0:1, :], units[1:2, :]
    bias = units[2:3, :]
    taps = [units[3 + tap : 4 + tap, :] for tap in range(KERNEL)]
    for flip, block in ((0, own_rows), (2, far_rows), (1, core_rows), (3, far_core_rows)):
        at = pl.multiple_of(lax.bitwise_xor(me, flip) * share, share)
        rows_held[pl.ds(at, share), :] = block[...]
    both = f32_dot(rows_held[...], gate_up[...])
    gate = both[:, :hidden] * gate_scale
    position = lax.broadcasted_iota(jnp.int32, gate.shape, 0)
    convolved = bias + gate * taps[KERNEL - 1]
    for back in range(1, KERNEL):
        moved = jnp.where(position >= back, pltpu.roll(gate, back, 0), 0.0)
        convolved += moved * taps[KERNEL - 1 - back]
    gelu = 0.5 * convolved * (1.0 + lax.erf(convolved * 0.5**0.5))
    active_held[...] = (gelu * (both[:, hidden:] * up_scale)).astype(jnp.bfloat16)
    picked = []
    for flip in (1, 3, 0, 2):
        at = pl.multiple_of(lax.bitwise_xor(me, flip) * share, share)
        picked.append(active_held[pl.ds(at, share), :])
    active = jnp.concatenate(picked, 0)
    step = 4 * LANES
    for at in range(0, down.shape[1], step):
        out = f32_dot(active, down[:, at : at + step]).astype(jnp.bfloat16)
        crossing[:, at : at + step] = out[: 2 * share]
        kept[:, at : at + step] = out[2 * share :]


def padded_columns(array, extra):
    return jnp.pad(array, [(0, 0)] * (array.ndim - 1) + [(0, extra)])


def local_fast(
    tokens,
    decay_logs,
    query_weight,
    key_weight,
    value_weight,
    out_weight,
    gate_weight,
    up_weight,
    down_weight,
    query_scale,
    key_scale,
    value_scale,
    out_scale,
    gate_scale,
    up_scale,
    down_scale,
    conv_weight,
    conv_bias,
    first_gain,
    first_bias,
    second_gain,
    second_bias,
):
    length, wide = tokens.shape
    tensors = lax.axis_size("tp")
    share = length // tensors
    line, me, half = lax.axis_index("fs"), lax.axis_index("tp"), lax.axis_index("grp")
    where = jnp.stack([line, me, half]).astype(jnp.int32)
    other_core, other_chip = exchange(tensors, 1), exchange(tensors, 2)

    rows = query_weight.shape[0] // 2
    columns = query_weight.shape[1] + key_weight.shape[1] + value_weight.shape[1]
    in_weights = (query_weight, key_weight, value_weight, out_weight)
    in_mine = half_call(where, 0, in_weights)
    in_other = half_call(where, 1, in_weights)
    in_pairs = line_gather(in_mine, line)

    small = jnp.concatenate([query_scale, key_scale, value_scale, out_scale, down_scale])
    arrived = [small] + [lax.ppermute(small, "fs", ring(step)) for step in (1, 2, 3)]
    table = jnp.zeros((PLACES,) + small.shape, small.dtype)
    for step, piece in enumerate(arrived):
        table = lax.dynamic_update_slice(
            table, piece[None], ((line - step) % PLACES, jnp.int32(0))
        )
    cuts, at = [], 0
    for part in (query_scale, key_scale, value_scale, out_scale, down_scale):
        cuts.append(table[:, at : at + part.shape[0]].reshape(1, -1))
        at += part.shape[0]
    in_scale = jnp.concatenate(cuts[:3], 1)
    out_factor, down_factor = cuts[3], cuts[4]

    hidden = gate_weight.shape[1] // PLACES
    extra = -hidden % LANES
    held = hidden + extra
    gate_own, gate_other, *gate_sends = kernel_call(
        gate_kernel,
        (bf16(rows + LANES, 2 * held),) * (PLACES + 1),
        where,
        (gate_weight, up_weight, down_weight),
        scratch=(pltpu.VMEM((PLACES, 2 * rows, 2 * held), jnp.bfloat16),),
        room=24,
    )
    gate_pieces = [gate_own, gate_other]
    for step in (1, 2, 3):
        piece = lax.ppermute(gate_sends[step - 1], "fs", ring(step))
        gate_pieces += [piece, swap(piece)]

    heads = query_weight.shape[1] // QK_HEAD
    angles = (
        jnp.arange(length, dtype=jnp.float32)[:, None]
        * (1.0 / angle_base ** jnp.linspace(0.0, 1.0, QK_HEAD // 2, dtype=jnp.float32))[None, :]
    )
    cosine = jnp.tile(jnp.repeat(jnp.cos(angles), 2, axis=1), (1, heads))
    sine = jnp.tile(
        jnp.repeat(jnp.sin(angles), 2, axis=1)
        * jnp.where(jnp.arange(QK_HEAD) % 2 == 0, -1.0, 1.0)[None, :],
        (1, heads),
    )
    cumulative = jnp.cumsum(decay_logs, axis=1)
    crossing, kept = kernel_call(
        retention_kernel,
        (bf16(2 * share, wide),) * 2,
        where,
        (tokens, in_scale, cosine, sine, cumulative, cumulative.T, in_mine, in_other)
        + sum(in_pairs, ()),
        flops=4 * length * wide * columns,
        scratch=(
            pltpu.VMEM((wide, columns), jnp.bfloat16),
            pltpu.VMEM((heads * V_HEAD, wide), jnp.bfloat16),
            pltpu.VMEM((length, heads * V_HEAD), jnp.bfloat16),
        ),
        room=28,
    )
    near_rows, far_rows = slice(0, share), slice(share, 2 * share)
    arrived = lax.ppermute(crossing, "tp", other_core)
    far = summed(kept, arrived, far_rows).astype(jnp.bfloat16)
    far = lax.ppermute(far, "tp", other_chip)
    first = norm_call(where, tokens, [kept, arrived, far], out_factor, first_gain, first_bias)

    gate_up, down = kernel_call(
        join_kernel, (bf16(wide, 2 * held), bf16(held, wide)), where, tuple(gate_pieces)
    )
    at = line * hidden
    units = jnp.concatenate(
        [gate_scale, up_scale, lax.dynamic_slice_in_dim(conv_bias, at, hidden, 0)]
    ).reshape(3, hidden)
    units = jnp.concatenate([units, lax.dynamic_slice_in_dim(conv_weight, at, hidden, 1)], 0)
    units = padded_columns(units, extra)
    totals = []
    for step in range(PLACES):
        rows_here = lax.ppermute(first, "fs", ring(step)) if step else first
        chip = lax.ppermute(rows_here, "tp", other_chip)
        core = lax.ppermute(rows_here, "tp", other_core)
        chip_core = lax.ppermute(chip, "tp", other_core)
        crossing, kept = kernel_call(
            feed_kernel,
            (bf16(2 * share, wide),) * 2,
            where,
            (rows_here, chip, core, chip_core, gate_up, down, units),
            flops=6 * length * wide * held,
            scratch=(
                pltpu.VMEM((length, wide), jnp.bfloat16),
                pltpu.VMEM((length, held), jnp.bfloat16),
            ),
        )
        arrived = lax.ppermute(crossing, "tp", other_core)
        far = summed(kept, arrived, far_rows).astype(jnp.bfloat16)
        far = lax.ppermute(far, "tp", other_chip)
        if step:
            total = summed(kept, arrived, near_rows) + far.astype(jnp.float32)
            total = lax.ppermute(total.astype(jnp.bfloat16), "fs", ring(PLACES - step))
            totals.append(total)
        else:
            totals += [kept, arrived, far]
    return norm_call(where, first, totals, down_factor, second_gain, second_bias)


def small_mesh(mesh):
    return mesh.shape["grp"] == 2 and mesh.shape["fs"] == PLACES and mesh.shape["tp"] == 4


def solution(mesh):
    in_specs = (
        P(("grp", "fs"), None),
        P("tp", ("grp", "fs")),
        P("fs", "tp"),
        P("fs", "tp"),
        P("fs", "tp"),
        P("tp", "fs"),
        P("fs", "tp"),
        P("fs", "tp"),
        P("tp", "fs"),
        P(("tp", "fs")),
        P(("tp", "fs")),
        P(("tp", "fs")),
        P("fs"),
        P(("tp", "fs")),
        P(("tp", "fs")),
        P("fs"),
        P(None, "tp"),
        P("tp"),
        P(),
        P(),
        P(),
        P(),
    )
    out_specs = P(("grp", "fs", "tp"), None)
    if not small_mesh(mesh):
        return jax.shard_map(
            local, mesh=mesh, in_specs=in_specs, out_specs=out_specs, check_vma=False
        )
    return jax.shard_map(
        local_fast,
        mesh=mesh,
        in_specs=in_specs,
        out_specs=out_specs,
        check_vma=False,
    )
```
